32 devices in a mesh: sp: 4 (over y, x), dp: 8 (over z, core).
Axes of the slice: x: 2, y: 2, z: 4, core: 2. Of those that a mesh axis runs over, the one named last changes fastest.
Arguments:
- tokens: bfloat16 [8, 768, 4096], P('dp', 'sp'), may hold values from -30 to 30
- query_weight: bfloat16 [4096, 512], P('dp', 'sp'), may hold values from -0.09375 to 0.09375
- key_weight: bfloat16 [4096, 512], P('dp', 'sp'), may hold values from -0.09375 to 0.09375
- value_weight: bfloat16 [4096, 512], P('dp', 'sp'), may hold values from -0.09375 to 0.09375
- cum_gate: float32 [8, 4, 768], P('dp', 'sp'), may hold values from -3072 to 0, as said below
Outputs:
- attended: bfloat16 [8, 768, 512], P('dp', 'sp')
The draws below stay inside these ranges and needn't reach their ends.
Inputs may be any that keep to these rules, and one draw needn't show every extreme that they name: `cum_gate`: never rising along positions; the first position holds one step's log gate.
All inputs are finite; a program needn't handle non-finite values.
Results may differ from the reference program's by a relative error of at most 0.0076.
The reference program's roundings to bfloat16 on the way count: a program that leaves them out, or rounds other values in their place, can miss the bound.
Values may be sent and summed in bfloat16 or wider, within the bound.
A program may use at most 128 MiB of HBM per device.

```python
import jax
import jax.numpy as jnp
from jax import lax

D = 4096
HEAD = 128
TOK_DEV = 192
HEADS = 4
WIDTH = 512
LEN = 768
SEQS = 8


def draw_tokens(key, part):
    base = jnp.clip(jax.random.normal(jax.random.fold_in(key, 11), (SEQS, LEN, D), jnp.float32), -6.0, 6.0)
    return base.astype(jnp.bfloat16)


def shared_matrix(key):
    return jax.random.normal(jax.random.fold_in(key, 21), (D, WIDTH), jnp.float32)


def draw_query_weight(key, part):
    return (jnp.clip(shared_matrix(key), -6.0, 6.0) / 64.0).astype(jnp.bfloat16)


def draw_key_weight(key, part):
    other = jax.random.normal(jax.random.fold_in(key, 22), (D, WIDTH), jnp.float32)
    return (jnp.clip(other, -6.0, 6.0) / 64.0).astype(jnp.bfloat16)


def draw_cum_gate(key, part):
    order = jax.random.permutation(jax.random.fold_in(key, 31), HEADS)
    slow = order < HEADS // 2
    rate = jnp.where(slow, 1.0 / LEN, 1.0 / 40.0)
    blocks = LEN // TOK_DEV
    block_factor = jnp.exp(jax.random.uniform(jax.random.fold_in(key, 32), (SEQS, HEADS, blocks, 1), jnp.float32, -0.69, 0.69))
    block_factor = jnp.broadcast_to(block_factor, (SEQS, HEADS, blocks, TOK_DEV)).reshape(SEQS, HEADS, LEN)
    step_factor = jax.random.uniform(jax.random.fold_in(key, 33), (SEQS, HEADS, LEN), jnp.float32, 0.2, 1.8)
    log_gate = -rate[None, :, None] * block_factor * step_factor
    return jnp.cumsum(log_gate, axis=2).astype(jnp.float32)


def block_scale(own_key, shape, shards, least, top_value):
    gain = 1.0
    for axis_at, shards_of in shards:
        steps = jax.random.uniform(jax.random.fold_in(jax.random.fold_in(own_key, 6), axis_at), (shards_of,), jnp.float32, least / len(shards), top_value / len(shards))
        gain = gain * jnp.repeat(jnp.exp(steps), shape[axis_at] // shards_of).reshape((-1,) + (1,) * (len(shape) - 1 - axis_at))
    return gain


def centred(key, shape, deviation, bound, cuts=(), dtype=jnp.bfloat16):
    values = deviation * jax.random.normal(key, shape, jnp.float32)
    if cuts:
        values = values * block_scale(key, shape, cuts, -0.22, 0.18)
    return jnp.clip(values, -bound, bound).astype(dtype)


def setup_inputs(seed: int = 0) -> dict:
    seeds = jax.random.split(jax.random.key(seed), 6)
    tokens = draw_tokens(jax.random.fold_in(seeds[5], 71), 0)
    query_weight = draw_query_weight(jax.random.fold_in(seeds[5], 71), 0)
    key_weight = draw_key_weight(jax.random.fold_in(seeds[5], 71), 0)
    value_weight = centred(seeds[3], (D, WIDTH), D ** -0.5, 0.09375, ((0, 8), (1, 4)))
    cum_gate = draw_cum_gate(jax.random.fold_in(seeds[5], 71), 0)
    return {"tokens": tokens, "query_weight": query_weight, "key_weight": key_weight, "value_weight": value_weight, "cum_gate": cum_gate}


block_rows = 512


def attend(queries, keys, values, gates):
    length = queries.shape[0]
    scale = queries.shape[1] ** -0.5
    pieces = []
    for start in range(0, length, block_rows):
        finish = min(start + block_rows, length)
        scores = jnp.dot(queries[start:finish], keys[:finish].T, preferred_element_type=jnp.float32) * scale
        scores = scores + gates[start:finish, None] - gates[None, :finish]
        rows_at = start + lax.broadcasted_iota(jnp.int32, scores.shape, 0)
        cols_at = lax.broadcasted_iota(jnp.int32, scores.shape, 1)
        scores = jnp.where(cols_at <= rows_at, scores, -1e30)
        top = jnp.max(scores, axis=1, keepdims=True)
        weights = jnp.exp(scores - top)
        total = jnp.sum(weights, axis=1, keepdims=True)
        summed = jnp.dot(weights.astype(jnp.bfloat16), values[:finish], preferred_element_type=jnp.float32)
        pieces.append((summed / total).astype(jnp.bfloat16))
    return jnp.concatenate(pieces, axis=0)


def reference(tokens, query_weight, key_weight, value_weight, cum_gate):
    def one_sequence(inputs):
        rows, gates = inputs
        queries = jnp.dot(rows, query_weight, preferred_element_type=jnp.float32).astype(jnp.bfloat16)
        keys = jnp.dot(rows, key_weight, preferred_element_type=jnp.float32).astype(jnp.bfloat16)
        values = jnp.dot(rows, value_weight, preferred_element_type=jnp.float32).astype(jnp.bfloat16)

        def by_head(array):
            return jnp.transpose(array.reshape(LEN, HEADS, HEAD), (1, 0, 2))

        heads_out = lax.map(lambda group: attend(group[0], group[1], group[2], group[3]),
                            (by_head(queries), by_head(keys), by_head(values), gates))
        return jnp.transpose(heads_out, (1, 0, 2)).reshape(LEN, HEADS * HEAD)

    return lax.map(one_sequence, (tokens, cum_gate))
```

```python
import functools
import math

import jax
import jax.numpy as jnp
from jax import lax
from jax.experimental import pallas as pl
from jax.experimental.pallas import tpu as pltpu
from jax.sharding import PartitionSpec as P

MESH = pl.DeviceIdType.MESH
block_rows = 256


def kernel(
    nx, ny, nz, cores,
    tok_hbm, wq_hbm, wk_hbm, wv_hbm, gate_ref, out_ref,
    xbuf, wbuf, qkv, qout, gcol, attn, obuf,
    lsem, xsend, xrecv, wrecv, upsem, downsem, psem, ysem, qsend, qrecv, osend, orecv,
):
    tok, depth = tok_hbm.shape
    head = wq_hbm.shape[1]
    group = nx * tok
    length = ny * group
    s, d = lax.axis_index("sp"), lax.axis_index("dp")
    y, x = s // nx, s % nx
    z, c = d // cores, d % cores

    loads = [
        pltpu.make_async_copy(ref, wbuf.at[y, d, :, pl.ds(i * head, head)], lsem.at[i])
        for i, ref in enumerate((wq_hbm, wk_hbm, wv_hbm))
    ]
    loads.append(pltpu.make_async_copy(tok_hbm, xbuf.at[x], lsem.at[3]))
    for load in loads:
        load.start()

    barrier = pltpu.get_barrier_semaphore()
    for k in range(1, nx * ny):
        pl.semaphore_signal(
            barrier, inc=1, device_id={"sp": (s + k) % (nx * ny)}, device_id_type=MESH
        )
    for k in range(1, nz):
        pl.semaphore_signal(
            barrier, inc=1, device_id={"dp": ((z + k) % nz) * cores + c}, device_id_type=MESH
        )
    if cores > 1:
        pl.semaphore_signal(
            barrier, inc=1, device_id={"dp": z * cores + 1 - c}, device_id_type=MESH
        )
    pl.semaphore_wait(barrier, nx * ny - 1 + nz - 1 + cores - 1)

    def send_tokens(j):
        return pltpu.make_async_remote_copy(
            src_ref=tok_hbm, dst_ref=xbuf.at[x],
            send_sem=xsend.at[j - 1], recv_sem=xrecv.at[x],
            device_id={"sp": y * nx + (x + j) % nx}, device_id_type=MESH,
        )

    for j in range(1, nx):
        send_tokens(j).start()

    def send_block(h, zb, sem, device):
        at = zb * cores + c
        return pltpu.make_async_remote_copy(
            src_ref=wbuf.at[h, at], dst_ref=wbuf.at[h, at],
            send_sem=sem, recv_sem=wrecv.at[h, at],
            device_id=device, device_id_type=MESH,
        )

    def up(zb):
        return send_block(y, zb, upsem.at[zb], {"dp": jnp.minimum(z + 1, nz - 1) * cores + c})

    def down(zb):
        return send_block(y, zb, downsem.at[zb], {"dp": jnp.maximum(z - 1, 0) * cores + c})

    def across(h, zb):
        return send_block(h, zb, psem.at[h, zb], {"dp": z * cores + 1 - c})

    def aside(k, zb):
        return send_block(y, zb, ysem.at[k - 1, zb], {"sp": ((y + k) % ny) * nx + x})

    def arrived(h, at):
        pltpu.make_async_remote_copy(
            src_ref=wbuf.at[h, at], dst_ref=wbuf.at[h, at],
            send_sem=lsem.at[0], recv_sem=wrecv.at[h, at],
            device_id={"sp": (s + 1) % (nx * ny)}, device_id_type=MESH,
        ).wait_recv()

    def spread(zb):
        for k in range(1, ny):
            aside(k, zb).start()
        if cores > 1:
            across(y, zb).start()

    for load in loads[:3]:
        load.wait()

    pl.when(z < nz - 1)(lambda: up(z).start())
    pl.when(z > 0)(lambda: down(z).start())
    spread(z)

    for start in range(0, length, 128):
        row = gate_ref[:, start : start + 128]
        gcol[start : start + 128, :] = jnp.broadcast_to(row, (128, 128)).T

    for t in range(1, nz):

        @pl.when(z - t >= 0)
        def _(t=t):
            arrived(y, (z - t) * cores + c)
            pl.when(z < nz - 1)(lambda: up(z - t).start())
            spread(z - t)

        @pl.when(z + t < nz)
        def _(t=t):
            arrived(y, (z + t) * cores + c)
            pl.when(z > 0)(lambda: down(z + t).start())
            spread(z + t)

    if cores > 1:
        for zb in range(nz):
            arrived(y, zb * cores + 1 - c)

    def project(i, h):
        weights = wbuf[h].reshape(depth, 3 * head)
        return jnp.dot(xbuf[i], weights, preferred_element_type=jnp.float32).astype(jnp.bfloat16)

    def own_rows(i):
        return pl.ds(pl.multiple_of(y * group + i * tok, tok), tok)

    loads[3].wait()
    qkv[own_rows(x), :] = project(x, y)

    def from_side(zb):
        for k in range(1, ny):
            other = (y + ny - k) % ny
            arrived(other, zb * cores + c)
            if cores > 1:
                across(other, zb).start()

    from_side(z)
    for t in range(1, nz):
        pl.when(z - t >= 0)(lambda t=t: from_side(z - t))
        pl.when(z + t < nz)(lambda t=t: from_side(z + t))
    if cores > 1:
        for k in range(1, ny):
            for zb in range(nz):
                arrived((y + k) % ny, zb * cores + 1 - c)

    def send_qkv(k, i):
        return pltpu.make_async_remote_copy(
            src_ref=qout.at[k - 1, i], dst_ref=qkv.at[own_rows(i)],
            send_sem=qsend.at[k - 1, i], recv_sem=qrecv.at[y, i],
            device_id={"sp": ((y + k) % ny) * nx + x}, device_id_type=MESH,
        )

    def swap(i):
        for k in range(1, ny):
            qout[k - 1, i] = project(i, (y + k) % ny)
            send_qkv(k, i).start()

    swap(x)
    for j in range(1, nx):
        i = (x + j) % nx
        pltpu.make_async_remote_copy(
            src_ref=tok_hbm, dst_ref=xbuf.at[i],
            send_sem=xsend.at[j - 1], recv_sem=xrecv.at[i],
            device_id={"sp": (s + 1) % (nx * ny)}, device_id_type=MESH,
        ).wait_recv()
        swap(i)
    for j in range(1, nx):
        i = (x + j) % nx
        qkv[own_rows(i), :] = project(i, y)
    for k in range(1, ny):
        other = (y + k) % ny
        for i in range(nx):
            rows = pl.ds(pl.multiple_of(other * group + i * tok, tok), tok)
            pltpu.make_async_remote_copy(
                src_ref=qout.at[k - 1, i], dst_ref=qkv.at[rows],
                send_sem=qsend.at[k - 1, i], recv_sem=qrecv.at[other, i],
                device_id={"sp": other * nx + x}, device_id_type=MESH,
            ).wait_recv()

    def send_out(to):
        return pltpu.make_async_remote_copy(
            src_ref=attn.at[pl.ds(to * tok, tok)],
            dst_ref=obuf.at[:, pl.ds(pl.multiple_of(s * head, head), head)],
            send_sem=osend.at[to], recv_sem=orecv.at[s],
            device_id={"sp": to}, device_id_type=MESH,
        )

    scale = head ** (-0.5)
    sent = 0
    for start in range(0, length, block_rows):
        finish = min(start + block_rows, length)
        scores = (
            lax.dot_general(
                qkv[start:finish, :head], qkv[:finish, head : 2 * head],
                (((1,), (1,)), ((), ())), preferred_element_type=jnp.float32,
            )
            * scale
        )
        scores = scores + gcol[start:finish, :1] - gate_ref[:, :finish]
        rows_at = start + lax.broadcasted_iota(jnp.int32, scores.shape, 0)
        cols_at = lax.broadcasted_iota(jnp.int32, scores.shape, 1)
        scores = jnp.where(cols_at <= rows_at, scores, -1e30)
        top = jnp.max(scores, axis=1, keepdims=True)
        weights = jnp.exp(scores - top)
        total = jnp.sum(weights, axis=1, keepdims=True)
        summed = jnp.dot(
            weights.astype(jnp.bfloat16), qkv[:finish, 2 * head :],
            preferred_element_type=jnp.float32,
        )
        attn[start:finish, :] = (summed / total).astype(jnp.bfloat16)
        while (sent + 1) * tok <= finish:

            @pl.when(s != sent)
            def _(to=sent):
                send_out(to).start()

            @pl.when(s == sent)
            def _(to=sent):
                obuf[:, pl.ds(pl.multiple_of(s * head, head), head)] = attn[
                    to * tok : (to + 1) * tok, :
                ]

            sent += 1

    for k in range(1, nx * ny):
        source = (s + k) % (nx * ny)
        pltpu.make_async_remote_copy(
            src_ref=attn.at[pl.ds(0, tok)],
            dst_ref=obuf.at[:, pl.ds(pl.multiple_of(source * head, head), head)],
            send_sem=osend.at[source], recv_sem=orecv.at[source],
            device_id={"sp": source}, device_id_type=MESH,
        ).wait_recv()
    out_ref[...] = obuf[...]

    for j in range(1, nx):
        send_tokens(j).wait_send()
    for zb in range(nz):
        pl.when((z < nz - 1) & (zb <= z))(lambda zb=zb: up(zb).wait_send())
        pl.when((z > 0) & (zb >= z))(lambda zb=zb: down(zb).wait_send())
        for k in range(1, ny):
            aside(k, zb).wait_send()
        if cores > 1:
            for h in range(ny):
                across(h, zb).wait_send()
    for k in range(1, ny):
        for i in range(nx):
            send_qkv(k, i).wait_send()
    for to in range(nx * ny):
        pl.when(s != to)(lambda to=to: send_out(to).wait_send())


def body(sp, dp, tokens, query_weight, key_weight, value_weight, cum_gate):
    nx = max(n for n in range(1, math.isqrt(sp) + 1) if sp % n == 0)
    ny = sp // nx
    cores = 2 if dp % 2 == 0 else 1
    nz = dp // cores
    tok, depth = tokens.shape[1:]
    rows, head = query_weight.shape
    length = sp * tok
    dma = pltpu.SemaphoreType.DMA
    anywhere = pl.BlockSpec(memory_space=pl.ANY)
    vmem = pl.BlockSpec(memory_space=pltpu.VMEM)
    out = pl.pallas_call(
        functools.partial(kernel, nx, ny, nz, cores),
        out_shape=jax.ShapeDtypeStruct((tok, sp * head), jnp.bfloat16),
        in_specs=[anywhere] * 4 + [vmem],
        out_specs=vmem,
        scratch_shapes=[
            pltpu.VMEM((nx, tok, depth), jnp.bfloat16),
            pltpu.VMEM((ny, dp, rows, 3 * head), jnp.bfloat16),
            pltpu.VMEM((length, 3 * head), jnp.bfloat16),
            pltpu.VMEM((ny - 1, nx, tok, 3 * head), jnp.bfloat16),
            pltpu.VMEM((length, 128), jnp.float32),
            pltpu.VMEM((length, head), jnp.bfloat16),
            pltpu.VMEM((tok, sp * head), jnp.bfloat16),
            dma((4,)),
            dma((nx - 1,)),
            dma((nx,)),
            dma((ny, dp)),
            dma((nz,)),
            dma((nz,)),
            dma((ny, nz)),
            dma((ny - 1, nz)),
            dma((ny - 1, nx)),
            dma((ny, nx)),
            dma((sp,)),
            dma((sp,)),
        ],
        compiler_params=pltpu.CompilerParams(
            collective_id=0, has_side_effects=True, vmem_limit_bytes=60 * 1024 * 1024
        ),
    )(tokens[0], query_weight, key_weight, value_weight, cum_gate[0])
    return out[None]


def solution(mesh):
    in_specs = (
        P("dp", "sp", None),
        P("dp", "sp"),
        P("dp", "sp"),
        P("dp", "sp"),
        P("dp", "sp", None),
    )
    out_specs = P("dp", "sp", None)
    return jax.shard_map(
        functools.partial(body, mesh.shape["sp"], mesh.shape["dp"]),
        mesh=mesh, in_specs=in_specs, out_specs=out_specs, check_vma=False,
    )
```

```python
import functools
import math

import jax
import jax.numpy as jnp
from jax import lax
from jax.experimental import pallas as pl
from jax.experimental.pallas import tpu as pltpu
from jax.sharding import PartitionSpec as P

MESH = pl.DeviceIdType.MESH
block_rows = 256


def kernel(
    nx, ny, nz, cores,
    tok_hbm, wq_hbm, wk_hbm, wv_hbm, gate_ref, out_ref,
    xbuf, wbuf, acc, qkv, qout, gcol, attn, obuf,
    lsem, tsem, xsend, xrecv, wrecv, upsem, downsem, upq, downq, psem, pq, ysem, yq,
    qsend, qrecv, osend, orecv,
):
    tok, depth = tok_hbm.shape
    rows, head = wq_hbm.shape
    early = rows // 4
    chunk = cores * rows
    group = nx * tok
    length = ny * group
    s, d = lax.axis_index("sp"), lax.axis_index("dp")
    y, x = s // nx, s % nx
    z, c = d // cores, d % cores

    def piece(zb):
        return tok_hbm.at[:, pl.ds(pl.multiple_of(zb * chunk, chunk), chunk)]

    loads = [
        pltpu.make_async_copy(ref, wbuf.at[y, d, :, pl.ds(i * head, head)], lsem.at[i])
        for i, ref in enumerate((wq_hbm, wk_hbm, wv_hbm))
    ]
    own_loads = [
        pltpu.make_async_copy(piece(zb), xbuf.at[x, zb], tsem.at[zb]) for zb in range(nz)
    ]
    for load in loads + own_loads:
        load.start()

    barrier = pltpu.get_barrier_semaphore()
    for k in range(1, nx * ny):
        pl.semaphore_signal(
            barrier, inc=1, device_id={"sp": (s + k) % (nx * ny)}, device_id_type=MESH
        )
    for k in range(1, nz):
        pl.semaphore_signal(
            barrier, inc=1, device_id={"dp": ((z + k) % nz) * cores + c}, device_id_type=MESH
        )
    if cores > 1:
        pl.semaphore_signal(
            barrier, inc=1, device_id={"dp": z * cores + 1 - c}, device_id_type=MESH
        )
    pl.semaphore_wait(barrier, nx * ny - 1 + nz - 1 + cores - 1)

    def step(t, act):
        if t == 0:
            act(z)
            return
        pl.when(z - t >= 0)(lambda: act(z - t))
        pl.when(z + t < nz)(lambda: act(z + t))

    def send_tokens(j, zb):
        return pltpu.make_async_remote_copy(
            src_ref=piece(zb), dst_ref=xbuf.at[x, zb],
            send_sem=xsend.at[j - 1, zb], recv_sem=xrecv.at[x, zb],
            device_id={"sp": y * nx + (x + j) % nx}, device_id_type=MESH,
        )

    def view(h, at, part):
        if part == 0:
            return wbuf.at[h, at]
        if part == 1:
            return wbuf.at[h, at, pl.ds(0, early)]
        return wbuf.at[h, at, pl.ds(early, rows - early)]

    def send_block(h, zb, part, sem, device):
        at = zb * cores + c
        return pltpu.make_async_remote_copy(
            src_ref=view(h, at, part), dst_ref=view(h, at, part),
            send_sem=sem, recv_sem=wrecv.at[int(part == 1), h, at],
            device_id=device, device_id_type=MESH,
        )

    above = {"dp": jnp.minimum(z + 1, nz - 1) * cores + c}
    below = {"dp": jnp.maximum(z - 1, 0) * cores + c}
    beside = {"dp": z * cores + 1 - c}

    def aside(k):
        return {"sp": ((y + k) % ny) * nx + x}

    def up(zb):
        return send_block(y, zb, 0, upsem.at[zb], above)

    def down(zb):
        return send_block(y, zb, 0, downsem.at[zb], below)

    def up_early(h, zb):
        return send_block(h, zb, 1, upq.at[h, zb], above)

    def down_early(h, zb):
        return send_block(h, zb, 1, downq.at[h, zb], below)

    def across(h, zb, part):
        return send_block(h, zb, part, (pq if part == 1 else psem).at[h, zb], beside)

    def side_early(k):
        return send_block(y, z, 1, yq.at[k - 1], aside(k))

    def side_late(k, zb):
        return send_block(y, zb, 2, ysem.at[k - 1, zb], aside(k))

    def arrived(h, at, part):
        pltpu.make_async_remote_copy(
            src_ref=view(h, at, part), dst_ref=view(h, at, part),
            send_sem=lsem.at[0], recv_sem=wrecv.at[int(part == 1), h, at],
            device_id={"sp": (s + 1) % (nx * ny)}, device_id_type=MESH,
        ).wait_recv()

    others = [(y + k) % ny for k in range(1, ny)]

    for load in loads:
        load.wait()

    def spread(zb):
        for k in range(1, ny):
            side_late(k, zb).start()
        if cores > 1:
            across(y, zb, 0).start()

    for k in range(1, ny):
        side_early(k).start()
    pl.when(z < nz - 1)(lambda: up(z).start())
    pl.when(z > 0)(lambda: down(z).start())
    for j in range(1, nx):
        send_tokens(j, z).start()
    spread(z)
    for t in range(1, nz):
        for j in range(1, nx):
            step(t, lambda zb, j=j: send_tokens(j, zb).start())

    for start in range(0, length, 128):
        row = gate_ref[:, start : start + 128]
        gcol[start : start + 128, :] = jnp.broadcast_to(row, (128, 128)).T
    acc[...] = jnp.zeros_like(acc)

    def relay(t):
        def from_below(zb):
            arrived(y, zb * cores + c, 0)
            pl.when(z < nz - 1)(lambda: up(zb).start())
            spread(zb)

        def from_above(zb):
            arrived(y, zb * cores + c, 0)
            pl.when(z > 0)(lambda: down(zb).start())
            spread(zb)

        def hand_on(zb, upward, downward):
            for h in others:
                arrived(h, zb * cores + c, 1)
                if upward:
                    pl.when(z < nz - 1)(lambda h=h: up_early(h, zb).start())
                if downward:
                    pl.when(z > 0)(lambda h=h: down_early(h, zb).start())
                if cores > 1:
                    across(h, zb, 1).start()

        if t == 0:
            hand_on(z, True, True)
            return
        pl.when(z - t >= 0)(lambda: from_below(z - t))
        pl.when(z + t < nz)(lambda: from_above(z + t))
        pl.when(z - t >= 0)(lambda: hand_on(z - t, True, False))
        pl.when(z + t < nz)(lambda: hand_on(z + t, False, True))

    def from_side(zb):
        for h in others:
            arrived(h, zb * cores + c, 2)
            if cores > 1:
                across(h, zb, 2).start()

    def add(zb, i):
        for h in others + [y]:
            weights = wbuf[h, pl.ds(zb * cores, cores)].reshape(chunk, 3 * head)
            acc[h, i] += jnp.dot(xbuf[i, zb], weights, preferred_element_type=jnp.float32)

    def add_own(zb):
        if cores > 1:
            at = zb * cores + 1 - c
            arrived(y, at, 0)
            for h in others:
                arrived(h, at, 1)
                arrived(h, at, 2)
        pltpu.make_async_copy(piece(zb), xbuf.at[x, zb], tsem.at[zb]).wait()
        add(zb, x)

    def add_other(zb):
        for j in range(1, nx):
            i = (x + j) % nx
            pltpu.make_async_remote_copy(
                src_ref=piece(zb), dst_ref=xbuf.at[i, zb],
                send_sem=xsend.at[j - 1, zb], recv_sem=xrecv.at[i, zb],
                device_id={"sp": (s + 1) % (nx * ny)}, device_id_type=MESH,
            ).wait_recv()
            add(zb, i)

    def own_rows(i):
        return pl.ds(pl.multiple_of(y * group + i * tok, tok), tok)

    def send_qkv(k, i):
        return pltpu.make_async_remote_copy(
            src_ref=qout.at[k - 1, i], dst_ref=qkv.at[own_rows(i)],
            send_sem=qsend.at[k - 1, i], recv_sem=qrecv.at[y, i],
            device_id=aside(k), device_id_type=MESH,
        )

    def swap(i):
        for k in range(1, ny):
            qout[k - 1, i] = acc[others[k - 1], i].astype(jnp.bfloat16)
            send_qkv(k, i).start()

    relay(0)
    for t in range(nz):
        if t + 1 < nz:
            relay(t + 1)
        step(t, from_side)
        step(t, add_own)
        if t == nz - 1:
            swap(x)
        step(t, add_other)
    for j in range(1, nx):
        swap((x + j) % nx)
    for i in range(nx):
        qkv[own_rows(i), :] = acc[y, i].astype(jnp.bfloat16)
    for k in range(1, ny):
        other = (y + k) % ny
        for i in range(nx):
            taken = pl.ds(pl.multiple_of(other * group + i * tok, tok), tok)
            pltpu.make_async_remote_copy(
                src_ref=qout.at[k - 1, i], dst_ref=qkv.at[taken],
                send_sem=qsend.at[k - 1, i], recv_sem=qrecv.at[other, i],
                device_id={"sp": other * nx + x}, device_id_type=MESH,
            ).wait_recv()

    def send_out(to):
        return pltpu.make_async_remote_copy(
            src_ref=attn.at[pl.ds(to * tok, tok)],
            dst_ref=obuf.at[:, pl.ds(pl.multiple_of(s * head, head), head)],
            send_sem=osend.at[to], recv_sem=orecv.at[s],
            device_id={"sp": to}, device_id_type=MESH,
        )

    scale = head ** (-0.5)
    sent = 0
    for start in range(0, length, block_rows):
        finish = min(start + block_rows, length)
        scores = (
            lax.dot_general(
                qkv[start:finish, :head], qkv[:finish, head : 2 * head],
                (((1,), (1,)), ((), ())), preferred_element_type=jnp.float32,
            )
            * scale
        )
        scores = scores + gcol[start:finish, :1] - gate_ref[:, :finish]
        rows_at = start + lax.broadcasted_iota(jnp.int32, scores.shape, 0)
        cols_at = lax.broadcasted_iota(jnp.int32, scores.shape, 1)
        scores = jnp.where(cols_at <= rows_at, scores, -1e30)
        top = jnp.max(scores, axis=1, keepdims=True)
        weights = jnp.exp(scores - top)
        total = jnp.sum(weights, axis=1, keepdims=True)
        summed = jnp.dot(
            weights.astype(jnp.bfloat16), qkv[:finish, 2 * head :],
            preferred_element_type=jnp.float32,
        )
        attn[start:finish, :] = (summed / total).astype(jnp.bfloat16)
        while (sent + 1) * tok <= finish:

            @pl.when(s != sent)
            def _(to=sent):
                send_out(to).start()

            @pl.when(s == sent)
            def _(to=sent):
                obuf[:, pl.ds(pl.multiple_of(s * head, head), head)] = attn[
                    to * tok : (to + 1) * tok, :
                ]

            sent += 1

    for k in range(1, nx * ny):
        source = (s + k) % (nx * ny)
        pltpu.make_async_remote_copy(
            src_ref=attn.at[pl.ds(0, tok)],
            dst_ref=obuf.at[:, pl.ds(pl.multiple_of(source * head, head), head)],
            send_sem=osend.at[source], recv_sem=orecv.at[source],
            device_id={"sp": source}, device_id_type=MESH,
        ).wait_recv()
    out_ref[...] = obuf[...]

    for zb in range(nz):
        for j in range(1, nx):
            send_tokens(j, zb).wait_send()
        upward = (z < nz - 1) & (zb <= z)
        downward = (z > 0) & (zb >= z)
        pl.when(upward)(lambda zb=zb: up(zb).wait_send())
        pl.when(downward)(lambda zb=zb: down(zb).wait_send())
        for h in others:
            pl.when(upward)(lambda h=h, zb=zb: up_early(h, zb).wait_send())
            pl.when(downward)(lambda h=h, zb=zb: down_early(h, zb).wait_send())
            if cores > 1:
                across(h, zb, 1).wait_send()
                across(h, zb, 2).wait_send()
        if cores > 1:
            across(y, zb, 0).wait_send()
        for k in range(1, ny):
            side_late(k, zb).wait_send()
    for k in range(1, ny):
        side_early(k).wait_send()
    for k in range(1, ny):
        for i in range(nx):
            send_qkv(k, i).wait_send()
    for to in range(nx * ny):
        pl.when(s != to)(lambda to=to: send_out(to).wait_send())


def body(sp, dp, tokens, query_weight, key_weight, value_weight, cum_gate):
    nx = max(n for n in range(1, math.isqrt(sp) + 1) if sp % n == 0)
    ny = sp // nx
    cores = 2 if dp % 2 == 0 else 1
    nz = dp // cores
    tok, depth = tokens.shape[1:]
    rows, head = query_weight.shape
    length = sp * tok
    dma = pltpu.SemaphoreType.DMA
    anywhere = pl.BlockSpec(memory_space=pl.ANY)
    vmem = pl.BlockSpec(memory_space=pltpu.VMEM)
    out = pl.pallas_call(
        functools.partial(kernel, nx, ny, nz, cores),
        out_shape=jax.ShapeDtypeStruct((tok, sp * head), jnp.bfloat16),
        in_specs=[anywhere] * 4 + [vmem],
        out_specs=vmem,
        scratch_shapes=[
            pltpu.VMEM((nx, nz, tok, cores * rows), jnp.bfloat16),
            pltpu.VMEM((ny, dp, rows, 3 * head), jnp.bfloat16),
            pltpu.VMEM((ny, nx, tok, 3 * head), jnp.float32),
            pltpu.VMEM((length, 3 * head), jnp.bfloat16),
            pltpu.VMEM((ny - 1, nx, tok, 3 * head), jnp.bfloat16),
            pltpu.VMEM((length, 128), jnp.float32),
            pltpu.VMEM((length, head), jnp.bfloat16),
            pltpu.VMEM((tok, sp * head), jnp.bfloat16),
            dma((3,)),
            dma((nz,)),
            dma((nx - 1, nz)),
            dma((nx, nz)),
            dma((2, ny, dp)),
            dma((nz,)),
            dma((nz,)),
            dma((ny, nz)),
            dma((ny, nz)),
            dma((ny, nz)),
            dma((ny, nz)),
            dma((ny - 1, nz)),
            dma((ny - 1,)),
            dma((ny - 1, nx)),
            dma((ny, nx)),
            dma((sp,)),
            dma((sp,)),
        ],
        compiler_params=pltpu.CompilerParams(
            collective_id=0, has_side_effects=True, vmem_limit_bytes=60 * 1024 * 1024
        ),
    )(tokens[0], query_weight, key_weight, value_weight, cum_gate[0])
    return out[None]


def solution(mesh):
    in_specs = (
        P("dp", "sp", None),
        P("dp", "sp"),
        P("dp", "sp"),
        P("dp", "sp"),
        P("dp", "sp", None),
    )
    out_specs = P("dp", "sp", None)
    return jax.shard_map(
        functools.partial(body, mesh.shape["sp"], mesh.shape["dp"]),
        mesh=mesh, in_specs=in_specs, out_specs=out_specs, check_vma=False,
    )
```

```python
import functools
import math

import jax
import jax.numpy as jnp
from jax import lax
from jax.experimental import pallas as pl
from jax.experimental.pallas import tpu as pltpu
from jax.sharding import PartitionSpec as P

MESH = pl.DeviceIdType.MESH
block_rows = 256


def kernel(
    nx, ny, nz, cores,
    tok_hbm, wq_hbm, wk_hbm, wv_hbm, gate_ref, out_ref,
    xbuf, wbuf, acc, qkv, qout, gcol, attn, obuf,
    lsem, tsem, xsend, xrecv, wrecv, upsem, downsem, upq, downq, psem, pq, ysem, yq,
    qsend, qrecv, osend, orecv,
):
    tok, depth = tok_hbm.shape
    rows, head = wq_hbm.shape
    early = rows // 16
    chunk = cores * rows
    group = nx * tok
    length = ny * group
    s, d = lax.axis_index("sp"), lax.axis_index("dp")
    y, x = s // nx, s % nx
    z, c = d // cores, d % cores

    def piece(zb):
        return tok_hbm.at[:, pl.ds(pl.multiple_of(zb * chunk, chunk), chunk)]

    loads = [
        pltpu.make_async_copy(ref, wbuf.at[y, d, :, pl.ds(i * head, head)], lsem.at[i])
        for i, ref in enumerate((wq_hbm, wk_hbm, wv_hbm))
    ]
    own_loads = [
        pltpu.make_async_copy(piece(zb), xbuf.at[x, zb], tsem.at[zb]) for zb in range(nz)
    ]
    for load in loads + own_loads:
        load.start()

    barrier = pltpu.get_barrier_semaphore()
    for k in range(1, nx * ny):
        pl.semaphore_signal(
            barrier, inc=1, device_id={"sp": (s + k) % (nx * ny)}, device_id_type=MESH
        )
    for k in range(1, nz):
        pl.semaphore_signal(
            barrier, inc=1, device_id={"dp": ((z + k) % nz) * cores + c}, device_id_type=MESH
        )
    if cores > 1:
        pl.semaphore_signal(
            barrier, inc=1, device_id={"dp": z * cores + 1 - c}, device_id_type=MESH
        )
    pl.semaphore_wait(barrier, nx * ny - 1 + nz - 1 + cores - 1)

    def step(t, act):
        if t == 0:
            act(z)
            return
        pl.when(z - t >= 0)(lambda: act(z - t))
        pl.when(z + t < nz)(lambda: act(z + t))

    def send_tokens(j, zb):
        return pltpu.make_async_remote_copy(
            src_ref=piece(zb), dst_ref=xbuf.at[x, zb],
            send_sem=xsend.at[j - 1, zb], recv_sem=xrecv.at[x, zb],
            device_id={"sp": y * nx + (x + j) % nx}, device_id_type=MESH,
        )

    def view(h, at, part):
        if part == 0:
            return wbuf.at[h, at]
        if part == 1:
            return wbuf.at[h, at, pl.ds(0, early)]
        return wbuf.at[h, at, pl.ds(early, rows - early)]

    def send_block(h, zb, part, sem, device):
        at = zb * cores + c
        return pltpu.make_async_remote_copy(
            src_ref=view(h, at, part), dst_ref=view(h, at, part),
            send_sem=sem, recv_sem=wrecv.at[int(part == 1), h, at],
            device_id=device, device_id_type=MESH,
        )

    above = {"dp": jnp.minimum(z + 1, nz - 1) * cores + c}
    below = {"dp": jnp.maximum(z - 1, 0) * cores + c}
    beside = {"dp": z * cores + 1 - c}

    def aside(k):
        return {"sp": ((y + k) % ny) * nx + x}

    def up(zb):
        return send_block(y, zb, 0, upsem.at[zb], above)

    def down(zb):
        return send_block(y, zb, 0, downsem.at[zb], below)

    def up_early(h, zb):
        return send_block(h, zb, 1, upq.at[h, zb], above)

    def down_early(h, zb):
        return send_block(h, zb, 1, downq.at[h, zb], below)

    def across(h, zb, part):
        return send_block(h, zb, part, (pq if part == 1 else psem).at[h, zb], beside)

    def side_early(k):
        return send_block(y, z, 1, yq.at[k - 1], aside(k))

    def side_late(k, zb):
        return send_block(y, zb, 2, ysem.at[k - 1, zb], aside(k))

    def arrived(h, at, part):
        pltpu.make_async_remote_copy(
            src_ref=view(h, at, part), dst_ref=view(h, at, part),
            send_sem=lsem.at[0], recv_sem=wrecv.at[int(part == 1), h, at],
            device_id={"sp": (s + 1) % (nx * ny)}, device_id_type=MESH,
        ).wait_recv()

    others = [(y + k) % ny for k in range(1, ny)]

    for load in loads:
        load.wait()

    def spread(zb):
        for k in range(1, ny):
            side_late(k, zb).start()
        if cores > 1:
            across(y, zb, 0).start()

    for k in range(1, ny):
        side_early(k).start()
    pl.when(z < nz - 1)(lambda: up(z).start())
    pl.when(z > 0)(lambda: down(z).start())
    for j in range(1, nx):
        send_tokens(j, z).start()
    spread(z)
    for t in range(1, nz):
        for j in range(1, nx):
            step(t, lambda zb, j=j: send_tokens(j, zb).start())

    for start in range(0, length, 128):
        row = gate_ref[:, start : start + 128]
        gcol[start : start + 128, :] = jnp.broadcast_to(row, (128, 128)).T
    acc[...] = jnp.zeros_like(acc)

    def relay(t):
        def from_below(zb):
            arrived(y, zb * cores + c, 0)
            pl.when(z < nz - 1)(lambda: up(zb).start())
            spread(zb)

        def from_above(zb):
            arrived(y, zb * cores + c, 0)
            pl.when(z > 0)(lambda: down(zb).start())
            spread(zb)

        def hand_on(zb, upward, downward):
            for h in others:
                arrived(h, zb * cores + c, 1)
                if upward:
                    pl.when(z < nz - 1)(lambda h=h: up_early(h, zb).start())
                if downward:
                    pl.when(z > 0)(lambda h=h: down_early(h, zb).start())
                if cores > 1:
                    across(h, zb, 1).start()

        if t == 0:
            hand_on(z, True, True)
            return
        pl.when(z - t >= 0)(lambda: from_below(z - t))
        pl.when(z + t < nz)(lambda: from_above(z + t))
        pl.when(z - t >= 0)(lambda: hand_on(z - t, True, False))
        pl.when(z + t < nz)(lambda: hand_on(z + t, False, True))

    def from_side(zb):
        for h in others:
            arrived(h, zb * cores + c, 2)
            if cores > 1:
                across(h, zb, 2).start()

    def add(zb, i):
        for h in others + [y]:
            weights = wbuf[h, pl.ds(zb * cores, cores)].reshape(chunk, 3 * head)
            acc[h, i] += jnp.dot(xbuf[i, zb], weights, preferred_element_type=jnp.float32)

    def add_own(zb):
        if cores > 1:
            at = zb * cores + 1 - c
            arrived(y, at, 0)
            for h in others:
                arrived(h, at, 1)
                arrived(h, at, 2)
        pltpu.make_async_copy(piece(zb), xbuf.at[x, zb], tsem.at[zb]).wait()
        add(zb, x)

    def add_other(zb):
        for j in range(1, nx):
            i = (x + j) % nx
            pltpu.make_async_remote_copy(
                src_ref=piece(zb), dst_ref=xbuf.at[i, zb],
                send_sem=xsend.at[j - 1, zb], recv_sem=xrecv.at[i, zb],
                device_id={"sp": (s + 1) % (nx * ny)}, device_id_type=MESH,
            ).wait_recv()
            add(zb, i)

    def own_rows(i):
        return pl.ds(pl.multiple_of(y * group + i * tok, tok), tok)

    def send_qkv(k, i):
        return pltpu.make_async_remote_copy(
            src_ref=qout.at[k - 1, i], dst_ref=qkv.at[own_rows(i)],
            send_sem=qsend.at[k - 1, i], recv_sem=qrecv.at[y, i],
            device_id=aside(k), device_id_type=MESH,
        )

    def swap(i):
        for k in range(1, ny):
            qout[k - 1, i] = acc[others[k - 1], i].astype(jnp.bfloat16)
            send_qkv(k, i).start()

    relay(0)
    for t in range(nz):
        if t + 1 < nz:
            relay(t + 1)
        step(t, from_side)
        step(t, add_own)
        if t == nz - 1:
            swap(x)
        step(t, add_other)
    for j in range(1, nx):
        swap((x + j) % nx)
    for i in range(nx):
        qkv[own_rows(i), :] = acc[y, i].astype(jnp.bfloat16)
    for k in range(1, ny):
        other = (y + k) % ny
        for i in range(nx):
            taken = pl.ds(pl.multiple_of(other * group + i * tok, tok), tok)
            pltpu.make_async_remote_copy(
                src_ref=qout.at[k - 1, i], dst_ref=qkv.at[taken],
                send_sem=qsend.at[k - 1, i], recv_sem=qrecv.at[other, i],
                device_id={"sp": other * nx + x}, device_id_type=MESH,
            ).wait_recv()

    def send_out(to):
        return pltpu.make_async_remote_copy(
            src_ref=attn.at[pl.ds(to * tok, tok)],
            dst_ref=obuf.at[:, pl.ds(pl.multiple_of(s * head, head), head)],
            send_sem=osend.at[to], recv_sem=orecv.at[s],
            device_id={"sp": to}, device_id_type=MESH,
        )

    scale = head ** (-0.5)
    sent = 0
    for start in range(0, length, block_rows):
        finish = min(start + block_rows, length)
        scores = (
            lax.dot_general(
                qkv[start:finish, :head], qkv[:finish, head : 2 * head],
                (((1,), (1,)), ((), ())), preferred_element_type=jnp.float32,
            )
            * scale
        )
        scores = scores + gcol[start:finish, :1] - gate_ref[:, :finish]
        rows_at = start + lax.broadcasted_iota(jnp.int32, scores.shape, 0)
        cols_at = lax.broadcasted_iota(jnp.int32, scores.shape, 1)
        scores = jnp.where(cols_at <= rows_at, scores, -1e30)
        top = jnp.max(scores, axis=1, keepdims=True)
        weights = jnp.exp(scores - top)
        total = jnp.sum(weights, axis=1, keepdims=True)
        summed = jnp.dot(
            weights.astype(jnp.bfloat16), qkv[:finish, 2 * head :],
            preferred_element_type=jnp.float32,
        )
        attn[start:finish, :] = (summed / total).astype(jnp.bfloat16)
        while (sent + 1) * tok <= finish:

            @pl.when(s != sent)
            def _(to=sent):
                send_out(to).start()

            @pl.when(s == sent)
            def _(to=sent):
                obuf[:, pl.ds(pl.multiple_of(s * head, head), head)] = attn[
                    to * tok : (to + 1) * tok, :
                ]

            sent += 1

    for k in range(1, nx * ny):
        source = (s + k) % (nx * ny)
        pltpu.make_async_remote_copy(
            src_ref=attn.at[pl.ds(0, tok)],
            dst_ref=obuf.at[:, pl.ds(pl.multiple_of(source * head, head), head)],
            send_sem=osend.at[source], recv_sem=orecv.at[source],
            device_id={"sp": source}, device_id_type=MESH,
        ).wait_recv()
    last = pltpu.make_async_copy(obuf, out_ref, lsem.at[0])
    last.start()

    for zb in range(nz):
        for j in range(1, nx):
            send_tokens(j, zb).wait_send()
        upward = (z < nz - 1) & (zb <= z)
        downward = (z > 0) & (zb >= z)
        pl.when(upward)(lambda zb=zb: up(zb).wait_send())
        pl.when(downward)(lambda zb=zb: down(zb).wait_send())
        for h in others:
            pl.when(upward)(lambda h=h, zb=zb: up_early(h, zb).wait_send())
            pl.when(downward)(lambda h=h, zb=zb: down_early(h, zb).wait_send())
            if cores > 1:
                across(h, zb, 1).wait_send()
                across(h, zb, 2).wait_send()
        if cores > 1:
            across(y, zb, 0).wait_send()
        for k in range(1, ny):
            side_late(k, zb).wait_send()
    for k in range(1, ny):
        side_early(k).wait_send()
    for k in range(1, ny):
        for i in range(nx):
            send_qkv(k, i).wait_send()
    for to in range(nx * ny):
        pl.when(s != to)(lambda to=to: send_out(to).wait_send())
    last.wait()


def body(sp, dp, tokens, query_weight, key_weight, value_weight, cum_gate):
    nx = max(n for n in range(1, math.isqrt(sp) + 1) if sp % n == 0)
    ny = sp // nx
    cores = 2 if dp % 2 == 0 else 1
    nz = dp // cores
    tok, depth = tokens.shape[1:]
    rows, head = query_weight.shape
    length = sp * tok
    dma = pltpu.SemaphoreType.DMA
    anywhere = pl.BlockSpec(memory_space=pl.ANY)
    vmem = pl.BlockSpec(memory_space=pltpu.VMEM)
    out = pl.pallas_call(
        functools.partial(kernel, nx, ny, nz, cores),
        out_shape=jax.ShapeDtypeStruct((tok, sp * head), jnp.bfloat16),
        in_specs=[anywhere] * 4 + [vmem],
        out_specs=anywhere,
        scratch_shapes=[
            pltpu.VMEM((nx, nz, tok, cores * rows), jnp.bfloat16),
            pltpu.VMEM((ny, dp, rows, 3 * head), jnp.bfloat16),
            pltpu.VMEM((ny, nx, tok, 3 * head), jnp.float32),
            pltpu.VMEM((length, 3 * head), jnp.bfloat16),
            pltpu.VMEM((ny - 1, nx, tok, 3 * head), jnp.bfloat16),
            pltpu.VMEM((length, 128), jnp.float32),
            pltpu.VMEM((length, head), jnp.bfloat16),
            pltpu.VMEM((tok, sp * head), jnp.bfloat16),
            dma((3,)),
            dma((nz,)),
            dma((nx - 1, nz)),
            dma((nx, nz)),
            dma((2, ny, dp)),
            dma((nz,)),
            dma((nz,)),
            dma((ny, nz)),
            dma((ny, nz)),
            dma((ny, nz)),
            dma((ny, nz)),
            dma((ny - 1, nz)),
            dma((ny - 1,)),
            dma((ny - 1, nx)),
            dma((ny, nx)),
            dma((sp,)),
            dma((sp,)),
        ],
        compiler_params=pltpu.CompilerParams(
            collective_id=0, has_side_effects=True, vmem_limit_bytes=60 * 1024 * 1024
        ),
    )(tokens[0], query_weight, key_weight, value_weight, cum_gate[0])
    return out[None]


def solution(mesh):
    in_specs = (
        P("dp", "sp", None),
        P("dp", "sp"),
        P("dp", "sp"),
        P("dp", "sp"),
        P("dp", "sp", None),
    )
    out_specs = P("dp", "sp", None)
    return jax.shard_map(
        functools.partial(body, mesh.shape["sp"], mesh.shape["dp"]),
        mesh=mesh, in_specs=in_specs, out_specs=out_specs, check_vma=False,
    )
```

```python
import functools
import math

import jax
import jax.numpy as jnp
from jax import lax
from jax.experimental import pallas as pl
from jax.experimental.pallas import tpu as pltpu
from jax.sharding import PartitionSpec as P

MESH = pl.DeviceIdType.MESH
block_rows = 128


def kernel(
    nx, ny, nz, cores,
    tok_hbm, wq_hbm, wk_hbm, wv_hbm, gate_ref, out_ref,
    xbuf, wbuf, acc, qkv, qout, gcol, attn, obuf,
    lsem, tsem, xsend, xrecv, wrecv, upsem, downsem, upq, downq, psem, pq, ysem, yq,
    qsend, qrecv, osend, orecv,
):
    tok, depth = tok_hbm.shape
    rows, head = wq_hbm.shape
    early = rows // 16
    chunk = cores * rows
    group = nx * tok
    length = ny * group
    s, d = lax.axis_index("sp"), lax.axis_index("dp")
    y, x = s // nx, s % nx
    z, c = d // cores, d % cores

    def piece(zb):
        return tok_hbm.at[:, pl.ds(pl.multiple_of(zb * chunk, chunk), chunk)]

    loads = [
        pltpu.make_async_copy(ref, wbuf.at[y, d, :, pl.ds(i * head, head)], lsem.at[i])
        for i, ref in enumerate((wq_hbm, wk_hbm, wv_hbm))
    ]
    own_loads = [
        pltpu.make_async_copy(piece(zb), xbuf.at[x, zb], tsem.at[zb]) for zb in range(nz)
    ]
    for load in loads + own_loads:
        load.start()

    barrier = pltpu.get_barrier_semaphore()
    for k in range(1, nx * ny):
        pl.semaphore_signal(
            barrier, inc=1, device_id={"sp": (s + k) % (nx * ny)}, device_id_type=MESH
        )
    for k in range(1, nz):
        pl.semaphore_signal(
            barrier, inc=1, device_id={"dp": ((z + k) % nz) * cores + c}, device_id_type=MESH
        )
    if cores > 1:
        pl.semaphore_signal(
            barrier, inc=1, device_id={"dp": z * cores + 1 - c}, device_id_type=MESH
        )
    pl.semaphore_wait(barrier, nx * ny - 1 + nz - 1 + cores - 1)

    def step(t, act):
        if t == 0:
            act(z)
            return
        pl.when(z - t >= 0)(lambda: act(z - t))
        pl.when(z + t < nz)(lambda: act(z + t))

    def send_tokens(j, zb):
        return pltpu.make_async_remote_copy(
            src_ref=piece(zb), dst_ref=xbuf.at[x, zb],
            send_sem=xsend.at[j - 1, zb], recv_sem=xrecv.at[x, zb],
            device_id={"sp": y * nx + (x + j) % nx}, device_id_type=MESH,
        )

    def view(h, at, part):
        if part == 0:
            return wbuf.at[h, at]
        if part == 1:
            return wbuf.at[h, at, pl.ds(0, early)]
        return wbuf.at[h, at, pl.ds(early, rows - early)]

    def send_block(h, zb, part, sem, device):
        at = zb * cores + c
        return pltpu.make_async_remote_copy(
            src_ref=view(h, at, part), dst_ref=view(h, at, part),
            send_sem=sem, recv_sem=wrecv.at[int(part == 1), h, at],
            device_id=device, device_id_type=MESH,
        )

    above = {"dp": jnp.minimum(z + 1, nz - 1) * cores + c}
    below = {"dp": jnp.maximum(z - 1, 0) * cores + c}
    beside = {"dp": z * cores + 1 - c}

    def aside(k):
        return {"sp": ((y + k) % ny) * nx + x}

    def up(zb):
        return send_block(y, zb, 0, upsem.at[zb], above)

    def down(zb):
        return send_block(y, zb, 0, downsem.at[zb], below)

    def up_early(h, zb):
        return send_block(h, zb, 1, upq.at[h, zb], above)

    def down_early(h, zb):
        return send_block(h, zb, 1, downq.at[h, zb], below)

    def across(h, zb, part):
        return send_block(h, zb, part, (pq if part == 1 else psem).at[h, zb], beside)

    def side_early(k):
        return send_block(y, z, 1, yq.at[k - 1], aside(k))

    def side_late(k, zb):
        return send_block(y, zb, 2, ysem.at[k - 1, zb], aside(k))

    def arrived(h, at, part):
        pltpu.make_async_remote_copy(
            src_ref=view(h, at, part), dst_ref=view(h, at, part),
            send_sem=lsem.at[0], recv_sem=wrecv.at[int(part == 1), h, at],
            device_id={"sp": (s + 1) % (nx * ny)}, device_id_type=MESH,
        ).wait_recv()

    others = [(y + k) % ny for k in range(1, ny)]

    for load in loads:
        load.wait()

    def spread(zb):
        for k in range(1, ny):
            side_late(k, zb).start()
        if cores > 1:
            across(y, zb, 0).start()

    for k in range(1, ny):
        side_early(k).start()
    pl.when(z < nz - 1)(lambda: up(z).start())
    pl.when(z > 0)(lambda: down(z).start())
    for j in range(1, nx):
        send_tokens(j, z).start()
    spread(z)
    for t in range(1, nz):
        for j in range(1, nx):
            step(t, lambda zb, j=j: send_tokens(j, zb).start())

    for start in range(0, length, 128):
        row = gate_ref[:, start : start + 128]
        gcol[start : start + 128, :] = jnp.broadcast_to(row, (128, 128)).T
    acc[...] = jnp.zeros_like(acc)

    def relay(t):
        def from_below(zb):
            arrived(y, zb * cores + c, 0)
            pl.when(z < nz - 1)(lambda: up(zb).start())
            spread(zb)

        def from_above(zb):
            arrived(y, zb * cores + c, 0)
            pl.when(z > 0)(lambda: down(zb).start())
            spread(zb)

        def hand_on(zb, upward, downward):
            for h in others:
                arrived(h, zb * cores + c, 1)
                if upward:
                    pl.when(z < nz - 1)(lambda h=h: up_early(h, zb).start())
                if downward:
                    pl.when(z > 0)(lambda h=h: down_early(h, zb).start())
                if cores > 1:
                    across(h, zb, 1).start()

        if t == 0:
            hand_on(z, True, True)
            return
        pl.when(z - t >= 0)(lambda: from_below(z - t))
        pl.when(z + t < nz)(lambda: from_above(z + t))
        pl.when(z - t >= 0)(lambda: hand_on(z - t, True, False))
        pl.when(z + t < nz)(lambda: hand_on(z + t, False, True))

    def from_side(zb):
        for h in others:
            arrived(h, zb * cores + c, 2)
            if cores > 1:
                across(h, zb, 2).start()

    def add(zb, i):
        for h in others + [y]:
            weights = wbuf[h, pl.ds(zb * cores, cores)].reshape(chunk, 3 * head)
            acc[h, i] += jnp.dot(xbuf[i, zb], weights, preferred_element_type=jnp.float32)

    def add_own(zb):
        if cores > 1:
            at = zb * cores + 1 - c
            arrived(y, at, 0)
            for h in others:
                arrived(h, at, 1)
                arrived(h, at, 2)
        pltpu.make_async_copy(piece(zb), xbuf.at[x, zb], tsem.at[zb]).wait()
        add(zb, x)

    def add_other(zb):
        for j in range(1, nx):
            i = (x + j) % nx
            pltpu.make_async_remote_copy(
                src_ref=piece(zb), dst_ref=xbuf.at[i, zb],
                send_sem=xsend.at[j - 1, zb], recv_sem=xrecv.at[i, zb],
                device_id={"sp": (s + 1) % (nx * ny)}, device_id_type=MESH,
            ).wait_recv()
            add(zb, i)

    def own_rows(i):
        return pl.ds(pl.multiple_of(y * group + i * tok, tok), tok)

    def send_qkv(k, i):
        return pltpu.make_async_remote_copy(
            src_ref=qout.at[k - 1, i], dst_ref=qkv.at[own_rows(i)],
            send_sem=qsend.at[k - 1, i], recv_sem=qrecv.at[y, i],
            device_id=aside(k), device_id_type=MESH,
        )

    def swap(i):
        for k in range(1, ny):
            qout[k - 1, i] = acc[others[k - 1], i].astype(jnp.bfloat16)
            send_qkv(k, i).start()

    relay(0)
    for t in range(nz):
        if t + 1 < nz:
            relay(t + 1)
        step(t, from_side)
        step(t, add_own)
        if t == nz - 1:
            swap(x)
        step(t, add_other)
    for j in range(1, nx):
        swap((x + j) % nx)
    for i in range(nx):
        qkv[own_rows(i), :] = acc[y, i].astype(jnp.bfloat16)
    for k in range(1, ny):
        other = (y + k) % ny
        for i in range(nx):
            taken = pl.ds(pl.multiple_of(other * group + i * tok, tok), tok)
            pltpu.make_async_remote_copy(
                src_ref=qout.at[k - 1, i], dst_ref=qkv.at[taken],
                send_sem=qsend.at[k - 1, i], recv_sem=qrecv.at[other, i],
                device_id={"sp": other * nx + x}, device_id_type=MESH,
            ).wait_recv()

    def send_out(to):
        return pltpu.make_async_remote_copy(
            src_ref=attn.at[pl.ds(to * tok, tok)],
            dst_ref=obuf.at[:, pl.ds(pl.multiple_of(s * head, head), head)],
            send_sem=osend.at[to], recv_sem=orecv.at[s],
            device_id={"sp": to}, device_id_type=MESH,
        )

    scale = head ** (-0.5)
    sent = 0
    for start in range(0, length, block_rows):
        finish = min(start + block_rows, length)
        scores = (
            lax.dot_general(
                qkv[start:finish, :head], qkv[:finish, head : 2 * head],
                (((1,), (1,)), ((), ())), preferred_element_type=jnp.float32,
            )
            * scale
        )
        scores = scores + gcol[start:finish, :1] - gate_ref[:, :finish]
        rows_at = start + lax.broadcasted_iota(jnp.int32, scores.shape, 0)
        cols_at = lax.broadcasted_iota(jnp.int32, scores.shape, 1)
        scores = jnp.where(cols_at <= rows_at, scores, -1e30)
        top = jnp.max(scores, axis=1, keepdims=True)
        weights = jnp.exp(scores - top)
        total = jnp.sum(weights, axis=1, keepdims=True)
        summed = jnp.dot(
            weights.astype(jnp.bfloat16), qkv[:finish, 2 * head :],
            preferred_element_type=jnp.float32,
        )
        attn[start:finish, :] = (summed / total).astype(jnp.bfloat16)
        while (sent + 1) * tok <= finish:

            @pl.when(s != sent)
            def _(to=sent):
                send_out(to).start()

            @pl.when(s == sent)
            def _(to=sent):
                obuf[:, pl.ds(pl.multiple_of(s * head, head), head)] = attn[
                    to * tok : (to + 1) * tok, :
                ]

            sent += 1

    for k in range(1, nx * ny):
        source = (s + k) % (nx * ny)
        pltpu.make_async_remote_copy(
            src_ref=attn.at[pl.ds(0, tok)],
            dst_ref=obuf.at[:, pl.ds(pl.multiple_of(source * head, head), head)],
            send_sem=osend.at[source], recv_sem=orecv.at[source],
            device_id={"sp": source}, device_id_type=MESH,
        ).wait_recv()
    last = pltpu.make_async_copy(obuf, out_ref, lsem.at[0])
    last.start()

    for zb in range(nz):
        for j in range(1, nx):
            send_tokens(j, zb).wait_send()
        upward = (z < nz - 1) & (zb <= z)
        downward = (z > 0) & (zb >= z)
        pl.when(upward)(lambda zb=zb: up(zb).wait_send())
        pl.when(downward)(lambda zb=zb: down(zb).wait_send())
        for h in others:
            pl.when(upward)(lambda h=h, zb=zb: up_early(h, zb).wait_send())
            pl.when(downward)(lambda h=h, zb=zb: down_early(h, zb).wait_send())
            if cores > 1:
                across(h, zb, 1).wait_send()
                across(h, zb, 2).wait_send()
        if cores > 1:
            across(y, zb, 0).wait_send()
        for k in range(1, ny):
            side_late(k, zb).wait_send()
    for k in range(1, ny):
        side_early(k).wait_send()
    for k in range(1, ny):
        for i in range(nx):
            send_qkv(k, i).wait_send()
    for to in range(nx * ny):
        pl.when(s != to)(lambda to=to: send_out(to).wait_send())
    last.wait()


def body(sp, dp, tokens, query_weight, key_weight, value_weight, cum_gate):
    nx = max(n for n in range(1, math.isqrt(sp) + 1) if sp % n == 0)
    ny = sp // nx
    cores = 2 if dp % 2 == 0 else 1
    nz = dp // cores
    tok, depth = tokens.shape[1:]
    rows, head = query_weight.shape
    length = sp * tok
    dma = pltpu.SemaphoreType.DMA
    anywhere = pl.BlockSpec(memory_space=pl.ANY)
    vmem = pl.BlockSpec(memory_space=pltpu.VMEM)
    out = pl.pallas_call(
        functools.partial(kernel, nx, ny, nz, cores),
        out_shape=jax.ShapeDtypeStruct((tok, sp * head), jnp.bfloat16),
        in_specs=[anywhere] * 4 + [vmem],
        out_specs=anywhere,
        scratch_shapes=[
            pltpu.VMEM((nx, nz, tok, cores * rows), jnp.bfloat16),
            pltpu.VMEM((ny, dp, rows, 3 * head), jnp.bfloat16),
            pltpu.VMEM((ny, nx, tok, 3 * head), jnp.float32),
            pltpu.VMEM((length, 3 * head), jnp.bfloat16),
            pltpu.VMEM((ny - 1, nx, tok, 3 * head), jnp.bfloat16),
            pltpu.VMEM((length, 128), jnp.float32),
            pltpu.VMEM((length, head), jnp.bfloat16),
            pltpu.VMEM((tok, sp * head), jnp.bfloat16),
            dma((3,)),
            dma((nz,)),
            dma((nx - 1, nz)),
            dma((nx, nz)),
            dma((2, ny, dp)),
            dma((nz,)),
            dma((nz,)),
            dma((ny, nz)),
            dma((ny, nz)),
            dma((ny, nz)),
            dma((ny, nz)),
            dma((ny - 1, nz)),
            dma((ny - 1,)),
            dma((ny - 1, nx)),
            dma((ny, nx)),
            dma((sp,)),
            dma((sp,)),
        ],
        compiler_params=pltpu.CompilerParams(
            collective_id=0, has_side_effects=True, vmem_limit_bytes=60 * 1024 * 1024
        ),
    )(tokens[0], query_weight, key_weight, value_weight, cum_gate[0])
    return out[None]


def solution(mesh):
    in_specs = (
        P("dp", "sp", None),
        P("dp", "sp"),
        P("dp", "sp"),
        P("dp", "sp"),
        P("dp", "sp", None),
    )
    out_specs = P("dp", "sp", None)
    return jax.shard_map(
        functools.partial(body, mesh.shape["sp"], mesh.shape["dp"]),
        mesh=mesh, in_specs=in_specs, out_specs=out_specs, check_vma=False,
    )
```
